32 devices in a mesh: rep: 2 (over x), fs: 8 (over z, y), tp: 2 (over core).
Axes of the slice: x: 2, y: 2, z: 4, core: 2. Of those that a mesh axis runs over, the one named last changes fastest.
Arguments:
- tokens: bfloat16 [12288, 2048], P(('rep', 'fs')), may hold values from -6 to 6
- norm_gain: float32 [2048], replicated, may hold values from 0.1 to 1.9
- up_weight: bfloat16 [2048, 8192], P('fs', 'tp'), may hold values from -0.125 to 0.125
- down_weight: bfloat16 [8192, 2048], P('tp', 'fs'), may hold values from -0.0625 to 0.0625
Outputs:
- layer_out: bfloat16 [12288, 2048], P(('rep', 'fs'), 'tp')
The draws below stay inside these ranges and needn't reach their ends.
All inputs are finite; a program needn't handle non-finite values.
Results may differ from the reference program's by a relative error of at most 0.013.
Values may be sent and summed in bfloat16 or wider, within the bound.
A program may use at most 128 MiB of HBM per device.

```python
import jax
import jax.numpy as jnp
from jax import lax

D = 2048
FF = 8192
TOK_GRP = 768
TOKENS = 12288
N_REP = 2
N_FS = 8
N_TP = 2


def block_scale(own_key, extent, split, smallest, high):
    gain, own = 1.0, jax.random.fold_in(own_key, 6)
    for dim, parts in split:
        draws = jnp.exp(jax.random.uniform(jax.random.fold_in(own, dim), (parts,), jnp.float32, smallest / len(split), high / len(split)))
        gain = gain * jnp.repeat(draws, extent[dim] // parts).reshape([-1 if axis == dim else 1 for axis in range(len(extent))])
    return gain


def gaussian(key, shape, scale, bound, cuts=(), dtype=jnp.bfloat16):
    entries = jax.random.normal(key, shape, jnp.float32) * scale
    if len(cuts) > 0:
        entries = block_scale(key, shape, cuts, -0.22, 0.18) * entries
    return jnp.clip(entries, min=-bound, max=bound).astype(dtype)


def setup_inputs(seed: int = 0) -> dict:
    seeds = jax.random.split(jax.random.key(seed), 5)
    return {
        "tokens": gaussian(seeds[0], (TOKENS, D), 1.0, 6.0, ((0, 16),)),
        "norm_gain": jnp.clip(1.0 + 0.18 * jax.random.normal(seeds[1], (D,), jnp.float32), 0.1, 1.9),
        "up_weight": gaussian(seeds[2], (D, FF), D ** -0.5, 0.125, ((0, 8), (1, 2))),
        "down_weight": gaussian(seeds[3], (FF, D), FF ** -0.5, 0.0625, ((0, 2), (1, 8))),
    }


def group_layer(rows, norm_gain, up_weight, down_weight):
    xf = rows.astype(jnp.float32)
    inv_rms = lax.rsqrt(lax.optimization_barrier(jnp.mean(xf * xf, axis=-1, keepdims=True)) + 1e-06)
    normed = (xf * inv_rms * norm_gain).astype(jnp.bfloat16)
    pre = jnp.dot(normed, up_weight, preferred_element_type=jnp.float32)
    hidden = jnp.square(jax.nn.relu(pre)).astype(jnp.bfloat16)
    width = hidden.shape[1] // N_TP
    total = xf
    for block in range(N_TP):
        partial_value = jnp.dot(hidden[:, block * width:(block + 1) * width], down_weight[block * width:(block + 1) * width], preferred_element_type=jnp.float32)
        total = total + partial_value.astype(jnp.bfloat16).astype(jnp.float32)
    return total.astype(jnp.bfloat16)

def reference(tokens, norm_gain, up_weight, down_weight):
    groups = tokens.reshape(N_REP * N_FS, TOK_GRP, D)
    result = lax.map(lambda rows: group_layer(rows, norm_gain, up_weight, down_weight), groups)
    return result.reshape(TOKENS, D)
```

```python
import jax
import jax.numpy as jnp
from jax import lax
from jax.sharding import PartitionSpec as P


def local(tokens, norm_gain, up_weight, down_weight):
    n_rep = lax.axis_size("rep")
    rep = lax.axis_index("rep")
    ff = up_weight.shape[1] // n_rep
    up = lax.all_gather(
        lax.dynamic_slice_in_dim(up_weight, rep * ff, ff, 1), "fs", axis=0, tiled=True)
    down = lax.all_gather(
        lax.dynamic_slice_in_dim(down_weight, rep * ff, ff, 0), "fs", axis=1, tiled=True)
    xf = tokens.astype(jnp.float32)
    inv_rms = lax.rsqrt(jnp.mean(xf * xf, axis=-1, keepdims=True) + 1e-06)
    normed = (xf * inv_rms * norm_gain).astype(jnp.bfloat16)
    normed = lax.all_gather(normed, "rep", axis=0, tiled=True)
    pre = jnp.dot(normed, up, preferred_element_type=jnp.float32)
    hidden = jnp.square(jax.nn.relu(pre)).astype(jnp.bfloat16)
    terms = jnp.dot(hidden, down, preferred_element_type=jnp.float32).astype(jnp.bfloat16)
    summed = lax.psum_scatter(terms, "tp", scatter_dimension=1, tiled=True)
    summed = lax.psum_scatter(summed, "rep", scatter_dimension=0, tiled=True).astype(jnp.float32)
    width = summed.shape[1]
    own_cols = lax.dynamic_slice_in_dim(xf, lax.axis_index("tp") * width, width, 1)
    return (own_cols + summed).astype(jnp.bfloat16)


def solution(mesh):
    placed = (P(("rep", "fs"), None), P(), P("fs", "tp"), P("tp", "fs"))
    return jax.shard_map(
        local, mesh=mesh, in_specs=placed, out_specs=P(("rep", "fs"), "tp"), check_vma=False
    )
```

```python
import functools

import jax
import jax.numpy as jnp
from jax import lax
from jax.experimental import pallas as pl
from jax.experimental.pallas import tpu as pltpu
from jax.sharding import PartitionSpec as P

MESH = pl.DeviceIdType.MESH
F32 = jnp.float32
BF16 = jnp.bfloat16


def kernel(nz, normed, up, down, out, T, acc, hid, U, Dn, Pr, Ar, Br, fin, loc, tok_s, tok_r,
           wy_s, wy_r, z_s, z_r, d_s, d_r, a_s, a_r, b_s, b_r, f_s, f_r):
    x, f, c = lax.axis_index("rep"), lax.axis_index("fs"), lax.axis_index("tp")
    z, y = f // 2, f % 2
    half, blk = T.shape[3], T.shape[4]
    wide = U.shape[2]
    row = blk // 2
    own = x * 2 + y
    ax, ay = (x + 1 - c) % 2, (y + c) % 2
    bx, by = (x + c) % 2, (y + 1 - c) % 2
    q_a, q_b, q_ab = ax * 2 + ay, bx * 2 + by, (1 - x) * 2 + 1 - y
    to_a = {"rep": ax, "fs": z * 2 + ay}
    to_b = {"rep": bx, "fs": z * 2 + by}
    to_y = {"fs": z * 2 + 1 - y}
    to_x = {"rep": 1 - x}
    to_c = {"tp": 1 - c}
    above = {"fs": jnp.minimum(z + 1, nz - 1) * 2 + y}
    below = {"fs": jnp.maximum(z - 1, 0) * 2 + y}
    has_above, has_below = z < nz - 1, z > 0

    def remote(src, dst, s, r, dev):
        return pltpu.make_async_remote_copy(
            src_ref=src, dst_ref=dst, send_sem=s, recv_sem=r, device_id=dev, device_id_type=MESH)

    def order(s):
        m = jnp.minimum(z, nz - 1 - z)
        near = z - (s + 1) // 2 if s % 2 else z + s // 2
        far = jnp.where(z < nz - 1 - z, s, nz - 1 - s)
        return jnp.where(s <= 2 * m, near, far)

    barrier = pltpu.get_barrier_semaphore()
    for dev in (to_x, to_y, to_c):
        pl.semaphore_signal(barrier, inc=1, device_id=dev, device_id_type=MESH)

    @pl.when(has_above)
    def _():
        pl.semaphore_signal(barrier, inc=1, device_id=above, device_id_type=MESH)

    @pl.when(has_below)
    def _():
        pl.semaphore_signal(barrier, inc=1, device_id=below, device_id_type=MESH)

    locals_ = []
    for k in range(nz):
        for h in range(2):
            locals_.append(pltpu.make_async_copy(
                normed.at[pl.ds(h * half, half), pl.ds(k * blk, blk)],
                T.at[k, own, h], loc.at[k * 2 + h]))
    slot = (lambda zz, p: U.at[zz, pl.ds(pl.multiple_of(p * row, row), row)],
            lambda zz, p: Dn.at[zz, :, pl.ds(pl.multiple_of(p * row, row), row)])
    part = (lambda q: up.at[:, pl.ds(pl.multiple_of(q * wide, wide), wide)],
            lambda q: down.at[pl.ds(pl.multiple_of(q * wide, wide), wide)])
    for w in range(2):
        locals_.append(pltpu.make_async_copy(part[w](own), slot[w](z, y), loc.at[2 * nz + w]))
    for copy in locals_:
        copy.start()
    pl.semaphore_wait(barrier, 3 + jnp.where(has_above, 1, 0) + jnp.where(has_below, 1, 0))

    swap = [remote(part[w](x * 2 + 1 - y), slot[w](z, y), wy_s.at[w], wy_r.at[w], to_y)
            for w in range(2)]

    def hop(w, upward, zz, p):
        return remote(slot[w](zz, p), slot[w](zz, p), z_s.at[w, 0 if upward else 1, zz, p],
                      z_r.at[w, zz, p], above if upward else below)

    def send(w, zz, p, act="start"):
        @pl.when(jnp.logical_and(has_above, zz <= z))
        def _():
            hop(w, True, zz, p).start() if act == "start" else hop(w, True, zz, p).wait_send()

        @pl.when(jnp.logical_and(has_below, zz >= z))
        def _():
            hop(w, False, zz, p).start() if act == "start" else hop(w, False, zz, p).wait_send()

    def pieces(w):
        return (y, 1 - y) if w == 0 else (0, 1)

    def arrive(w, s):
        zz = order(s)
        for p in pieces(w):
            hop(w, True, zz, p).wait_recv()
            send(w, zz, p)

    def piece(q):
        return T.at[:, q, c]

    tok = [remote(piece(own), piece(own), tok_s.at[0], tok_r.at[0], to_a),
           remote(piece(own), piece(own), tok_s.at[1], tok_r.at[1], to_b),
           remote(piece(q_a), piece(q_a), tok_s.at[2], tok_r.at[2], to_b)]
    tok += [remote(piece(q), piece(q), tok_s.at[3 + i], tok_r.at[3 + i], to_c)
            for i, q in enumerate((q_a, q_b, q_ab))]

    swap[0].start()
    locals_[2 * nz].wait()
    send(0, z, y)
    for copy in locals_[:2 * nz]:
        copy.wait()
    tok[0].start()
    tok[1].start()
    swap[1].start()
    swap[0].wait_recv()
    send(0, z, 1 - y)
    arrive(0, 1)
    tok[0].wait_recv()
    tok[2].start()
    tok[3].start()
    tok[1].wait_recv()
    tok[4].start()
    for s in range(2, nz - 1):
        arrive(0, s)
    locals_[2 * nz + 1].wait()
    swap[1].wait_recv()
    send(1, z, 0)
    send(1, z, 1)
    tok[2].wait_recv()
    tok[5].start()
    for i in range(3):
        tok[3 + i].wait_recv()
    for copy in tok:
        copy.wait_send()
    if nz > 2:
        arrive(1, 1)

    def up_block(s):
        zz = order(s)

        @pl.loop(0, 8)
        def _(i):
            q, h = i // 2, i % 2
            term = jnp.dot(T[zz, q, h], U[zz], preferred_element_type=F32)
            if s > 0:
                term += acc[q, h]
            if s < nz - 1:
                acc[q, h] = term
            else:
                hid[q, h] = jnp.square(jnp.maximum(term, 0.0)).astype(BF16)

    for s in range(nz):
        if s == nz - 1:
            arrive(0, s)
        up_block(s)

    def stage_a(s):
        zz = order(s)
        for h in (1 - c, c):
            @pl.loop(0, 4)
            def _(q):
                T[zz, q, h] = jnp.dot(
                    hid[q, h], Dn[zz], preferred_element_type=F32).astype(BF16)
            if h is not c:
                d2d(s).start()

    def d2d(s):
        zz = order(s)
        return remote(T.at[zz, :, 1 - c], Pr.at[zz], d_s.at[zz], d_r.at[zz], to_c)

    def to_first(s, i):
        zz = order(s)
        return remote(T.at[zz, (q_a, q_ab)[i], c], Ar.at[zz, i], a_s.at[zz, i], a_r.at[zz, i],
                      to_a)

    def to_second(s):
        zz = order(s)
        return remote(T.at[zz, q_b, c], Br.at[zz], b_s.at[zz], b_r.at[zz], to_b)

    def finish(s):
        zz = order(s)
        return remote(T.at[zz, own, c], fin.at[zz % (nz // 2), c], f_s.at[zz], f_r.at[zz], to_c)

    def stage_b(s):
        zz = order(s)
        d2d(s).wait_recv()
        for i, q in ((1, q_ab), (0, q_a), (2, q_b), (3, own)):
            T[zz, q, c] = (T[zz, q, c].astype(F32) + Pr[zz, q].astype(F32)).astype(BF16)
            if i < 2:
                to_first(s, i).start()

    def stage_c(s):
        zz = order(s)
        to_first(s, 1).wait_recv()
        T[zz, q_b, c] = (T[zz, q_b, c].astype(F32) + Ar[zz, 1].astype(F32)).astype(BF16)
        to_second(s).start()

    def stage_d(s):
        zz = order(s)
        to_first(s, 0).wait_recv()
        to_second(s).wait_recv()
        T[zz, own, c] = (T[zz, own, c].astype(F32) + Ar[zz, 0].astype(F32)
                         + Br[zz].astype(F32)).astype(BF16)

        @pl.when(zz // (nz // 2) == c)
        def _():
            fin[zz % (nz // 2), c] = T[zz, own, c]

        @pl.when(zz // (nz // 2) != c)
        def _():
            finish(s).start()

    for s in range(nz):
        if s > 1 or (s == 1 and nz == 2):
            arrive(1, s)
        stage_a(s)
        if s:
            stage_c(s - 1)
        stage_b(s)
        if s:
            stage_d(s - 1)
    stage_c(nz - 1)
    stage_d(nz - 1)

    for s in range(nz):
        zz = order(s)

        @pl.when(zz // (nz // 2) == c)
        def _():
            finish(s).wait_recv()

        @pl.when(zz // (nz // 2) != c)
        def _():
            finish(s).wait_send()
    outs = [pltpu.make_async_copy(
        fin.at[k, h], out.at[pl.ds(h * half, half), pl.ds(k * blk, blk)], loc.at[k * 2 + h])
        for k in range(nz // 2) for h in range(2)]
    for copy in outs:
        copy.start()
    for w in range(2):
        swap[w].wait_send()
        for s in range(nz):
            for p in pieces(w):
                send(w, order(s), p, "wait")
    for s in range(nz):
        d2d(s).wait_send()
        to_first(s, 0).wait_send()
        to_first(s, 1).wait_send()
        to_second(s).wait_send()
    for copy in outs:
        copy.wait()


def fused(nz, normed, up, down):
    rows, d = normed.shape
    wide = up.shape[1] // 4
    half, blk = rows // 2, d // nz
    sem = pltpu.SemaphoreType.DMA
    return pl.pallas_call(
        functools.partial(kernel, nz),
        out_shape=jax.ShapeDtypeStruct((rows, d // 2), BF16),
        in_specs=[pl.BlockSpec(memory_space=pl.ANY)] * 3,
        out_specs=pl.BlockSpec(memory_space=pl.ANY),
        scratch_shapes=[
            pltpu.VMEM((nz, 4, 2, half, blk), BF16),
            pltpu.VMEM((4, 2, half, wide), F32),
            pltpu.VMEM((4, 2, half, wide), BF16),
            pltpu.VMEM((nz, blk, wide), BF16),
            pltpu.VMEM((nz, wide, blk), BF16),
            pltpu.VMEM((nz, 4, half, blk), BF16),
            pltpu.VMEM((nz, 2, half, blk), BF16),
            pltpu.VMEM((nz, half, blk), BF16),
            pltpu.VMEM((nz // 2, 2, half, blk), BF16),
            sem((2 * nz + 2,)), sem((6,)), sem((6,)), sem((2,)), sem((2,)),
            sem((2, 2, nz, 2)), sem((2, nz, 2)), sem((nz,)), sem((nz,)),
            sem((nz, 2)), sem((nz, 2)), sem((nz,)), sem((nz,)), sem((nz,)), sem((nz,)),
        ],
        compiler_params=pltpu.CompilerParams(
            collective_id=0, has_side_effects=True, vmem_limit_bytes=60 * 2**20),
    )(normed, up, down)


def spread(normed, up_weight, down_weight):
    n_rep = lax.axis_size("rep")
    rep = lax.axis_index("rep")
    ff = up_weight.shape[1] // n_rep
    up = lax.all_gather(
        lax.dynamic_slice_in_dim(up_weight, rep * ff, ff, 1), "fs", axis=0, tiled=True)
    down = lax.all_gather(
        lax.dynamic_slice_in_dim(down_weight, rep * ff, ff, 0), "fs", axis=1, tiled=True)
    normed = lax.all_gather(normed, "rep", axis=0, tiled=True)
    pre = jnp.dot(normed, up, preferred_element_type=F32)
    hidden = jnp.square(jax.nn.relu(pre)).astype(BF16)
    terms = jnp.dot(hidden, down, preferred_element_type=F32).astype(BF16)
    summed = lax.psum_scatter(terms, "tp", scatter_dimension=1, tiled=True)
    return lax.psum_scatter(summed, "rep", scatter_dimension=0, tiled=True)


def local(tokens, norm_gain, up_weight, down_weight):
    xf = tokens.astype(F32)
    inv_rms = lax.rsqrt(jnp.mean(xf * xf, axis=-1, keepdims=True) + 1e-06)
    normed = (xf * inv_rms * norm_gain).astype(BF16)
    n_rep, n_fs, n_tp = (lax.axis_size(a) for a in ("rep", "fs", "tp"))
    if n_rep == 2 and n_tp == 2 and n_fs % 4 == 0:
        summed = fused(n_fs // 2, normed, up_weight, down_weight)
    else:
        summed = spread(normed, up_weight, down_weight)
    summed = summed.astype(F32)
    width = summed.shape[1]
    own_cols = lax.dynamic_slice_in_dim(xf, lax.axis_index("tp") * width, width, 1)
    return (own_cols + summed).astype(BF16)


def solution(mesh):
    placed = (P(("rep", "fs"), None), P(), P("fs", "tp"), P("tp", "fs"))
    return jax.shard_map(
        local, mesh=mesh, in_specs=placed, out_specs=P(("rep", "fs"), "tp"), check_vma=False
    )
```

```python
import functools

import jax
import jax.numpy as jnp
from jax import lax
from jax.experimental import pallas as pl
from jax.experimental.pallas import tpu as pltpu
from jax.sharding import PartitionSpec as P

MESH = pl.DeviceIdType.MESH
F32 = jnp.float32
BF16 = jnp.bfloat16


def kernel(nz, normed, up, down, out, T, acc, hid, U, Dn, Pr, Ar, Br, fin, loc, tok_s, tok_r,
           wy_s, wy_r, z_s, z_r, d_s, d_r, a_s, a_r, b_s, b_r, f_s, f_r):
    x, f, c = lax.axis_index("rep"), lax.axis_index("fs"), lax.axis_index("tp")
    z, y = f // 2, f % 2
    half, blk = T.shape[3], T.shape[4]
    wide = U.shape[2]
    row = blk // 2
    own = x * 2 + y
    ax, ay = (x + 1 - c) % 2, (y + c) % 2
    bx, by = (x + c) % 2, (y + 1 - c) % 2
    q_a, q_b, q_ab = ax * 2 + ay, bx * 2 + by, (1 - x) * 2 + 1 - y
    to_a = {"rep": ax, "fs": z * 2 + ay}
    to_b = {"rep": bx, "fs": z * 2 + by}
    to_y = {"fs": z * 2 + 1 - y}
    to_x = {"rep": 1 - x}
    to_c = {"tp": 1 - c}
    above = {"fs": jnp.minimum(z + 1, nz - 1) * 2 + y}
    below = {"fs": jnp.maximum(z - 1, 0) * 2 + y}
    has_above, has_below = z < nz - 1, z > 0

    def remote(src, dst, s, r, dev):
        return pltpu.make_async_remote_copy(
            src_ref=src, dst_ref=dst, send_sem=s, recv_sem=r, device_id=dev, device_id_type=MESH)

    def order(s):
        m = jnp.minimum(z, nz - 1 - z)
        near = z - (s + 1) // 2 if s % 2 else z + s // 2
        far = jnp.where(z < nz - 1 - z, s, nz - 1 - s)
        return jnp.where(s <= 2 * m, near, far)

    barrier = pltpu.get_barrier_semaphore()
    for dev in (to_x, to_y, to_c):
        pl.semaphore_signal(barrier, inc=1, device_id=dev, device_id_type=MESH)

    @pl.when(has_above)
    def _():
        pl.semaphore_signal(barrier, inc=1, device_id=above, device_id_type=MESH)

    @pl.when(has_below)
    def _():
        pl.semaphore_signal(barrier, inc=1, device_id=below, device_id_type=MESH)

    locals_ = []
    for k in range(nz):
        for h in range(2):
            locals_.append(pltpu.make_async_copy(
                normed.at[pl.ds(h * half, half), pl.ds(k * blk, blk)],
                T.at[k, own, h], loc.at[k * 2 + h]))
    slot = (lambda zz, p: U.at[zz, pl.ds(pl.multiple_of(p * row, row), row)],
            lambda zz, p: Dn.at[zz, :, pl.ds(pl.multiple_of(p * row, row), row)])
    part = (lambda q: up.at[:, pl.ds(pl.multiple_of(q * wide, wide), wide)],
            lambda q: down.at[pl.ds(pl.multiple_of(q * wide, wide), wide)])
    for w in range(2):
        locals_.append(pltpu.make_async_copy(part[w](own), slot[w](z, y), loc.at[2 * nz + w]))
    for copy in locals_:
        copy.start()
    pl.semaphore_wait(barrier, 3 + jnp.where(has_above, 1, 0) + jnp.where(has_below, 1, 0))

    swap = [remote(part[w](x * 2 + 1 - y), slot[w](z, y), wy_s.at[w], wy_r.at[w], to_y)
            for w in range(2)]

    def hop(w, upward, zz, p):
        return remote(slot[w](zz, p), slot[w](zz, p), z_s.at[w, 0 if upward else 1, zz, p],
                      z_r.at[w, zz, p], above if upward else below)

    def send(w, zz, p, act="start"):
        @pl.when(jnp.logical_and(has_above, zz <= z))
        def _():
            hop(w, True, zz, p).start() if act == "start" else hop(w, True, zz, p).wait_send()

        @pl.when(jnp.logical_and(has_below, zz >= z))
        def _():
            hop(w, False, zz, p).start() if act == "start" else hop(w, False, zz, p).wait_send()

    inner = jnp.logical_and(has_above, has_below)

    def pieces(w):
        return (y, 1 - y) if w == 0 else (0, 1)

    def relay(w, s):
        if s < nz:
            zz = order(s)
            for p in pieces(w):
                @pl.when(inner)
                def _():
                    hop(w, True, zz, p).wait_recv()
                send(w, zz, p)

    def arrived(w, s, p):
        @pl.when(jnp.logical_not(inner))
        def _():
            hop(w, True, order(s), p).wait_recv()

    def piece(q):
        return T.at[:, q, c]

    tok = [remote(piece(own), piece(own), tok_s.at[0], tok_r.at[0], to_a),
           remote(piece(own), piece(own), tok_s.at[1], tok_r.at[1], to_b),
           remote(piece(q_a), piece(q_a), tok_s.at[2], tok_r.at[2], to_b)]
    tok += [remote(piece(q), piece(q), tok_s.at[3 + i], tok_r.at[3 + i], to_c)
            for i, q in enumerate((q_a, q_b, q_ab))]

    def up_block(q, s):
        zz = order(s)

        @pl.loop(0, 2)
        def _(h):
            term = jnp.dot(T[zz, q, h], U[zz], preferred_element_type=F32)
            if s > 0:
                term += acc[q, h]
            if s < nz - 1:
                acc[q, h] = term
            else:
                hid[q, h] = jnp.square(jnp.maximum(term, 0.0)).astype(BF16)

    swap[0].start()
    swap[1].start()
    locals_[2 * nz].wait()
    send(0, z, y)
    for copy in locals_[:2 * nz]:
        copy.wait()
    tok[0].start()
    tok[1].start()
    swap[0].wait_recv()
    send(0, z, 1 - y)
    relay(0, 1)
    relay(0, 2)
    tok[0].wait_recv()
    tok[2].start()
    tok[3].start()
    locals_[2 * nz + 1].wait()
    swap[1].wait_recv()
    for s in range(3, nz):
        relay(0, s)
    send(1, z, 0)
    send(1, z, 1)
    up_block(own, 0)
    for p in pieces(0):
        arrived(0, 1, p)
    up_block(own, 1)
    tok[1].wait_recv()
    tok[4].start()
    for q, i in ((q_a, 4), (q_b, 3)):
        tok[i].wait_recv()
        up_block(q, 0)
        up_block(q, 1)
    relay(1, 1)
    for s in range(2, nz):
        for p in pieces(0):
            arrived(0, s, p)
        if s < nz - 1:
            for q in (own, q_a, q_b):
                up_block(q, s)
    relay(1, 2)
    tok[2].wait_recv()
    tok[5].start()
    if nz > 2:
        for q in (own, q_a, q_b):
            up_block(q, nz - 1)
    tok[5].wait_recv()
    for s in range(nz):
        up_block(q_ab, s)
    for s in range(3, nz):
        relay(1, s)
    for copy in tok:
        copy.wait_send()

    def cols(p):
        return pl.ds(p * row, row)

    def d2d(s, p):
        zz = order(s)
        return remote(T.at[zz, :, 1 - c, :, cols(p)], Pr.at[zz, :, :, cols(p)],
                      d_s.at[zz, p], d_r.at[zz, p], to_c)

    def to_first(s, p, i):
        zz = order(s)
        return remote(T.at[zz, (q_a, q_ab)[i], c, :, cols(p)], Ar.at[zz, i, :, cols(p)],
                      a_s.at[zz, p, i], a_r.at[zz, p, i], to_a)

    def to_second(s, p):
        zz = order(s)
        return remote(T.at[zz, q_b, c, :, cols(p)], Br.at[zz, :, cols(p)],
                      b_s.at[zz, p], b_r.at[zz, p], to_b)

    def finish(s, p):
        zz = order(s)
        return remote(T.at[zz, own, c, :, cols(p)], fin.at[zz % (nz // 2), c, :, cols(p)],
                      f_s.at[zz, p], f_r.at[zz, p], to_c)

    def stage_a(s, p):
        zz = order(s)
        for h in (1 - c, c):
            @pl.loop(0, 4)
            def _(q):
                T[zz, q, h, :, cols(p)] = jnp.dot(
                    hid[q, h], Dn[zz, :, cols(p)], preferred_element_type=F32).astype(BF16)
            if h is not c:
                d2d(s, p).start()

    def stage_b(s, p):
        zz, k = order(s), cols(p)
        d2d(s, p).wait_recv()
        for i, q in ((1, q_ab), (0, q_a), (2, q_b), (3, own)):
            T[zz, q, c, :, k] = (
                T[zz, q, c, :, k].astype(F32) + Pr[zz, q, :, k].astype(F32)).astype(BF16)
            if i < 2:
                to_first(s, p, i).start()

    def stage_c(s, p):
        zz, k = order(s), cols(p)
        to_first(s, p, 1).wait_recv()
        T[zz, q_b, c, :, k] = (
            T[zz, q_b, c, :, k].astype(F32) + Ar[zz, 1, :, k].astype(F32)).astype(BF16)
        to_second(s, p).start()

    def stage_d(s, p):
        zz, k = order(s), cols(p)
        to_first(s, p, 0).wait_recv()
        to_second(s, p).wait_recv()
        T[zz, own, c, :, k] = (
            T[zz, own, c, :, k].astype(F32) + Ar[zz, 0, :, k].astype(F32)
            + Br[zz, :, k].astype(F32)).astype(BF16)

        @pl.when(zz // (nz // 2) == c)
        def _():
            fin[zz % (nz // 2), c, :, k] = T[zz, own, c, :, k]

        @pl.when(zz // (nz // 2) != c)
        def _():
            finish(s, p).start()

    steps = [(s, p) for s in range(nz) for p in range(2)]
    for n, (s, p) in enumerate(steps):
        if s:
            arrived(1, s, p)
        stage_a(s, p)
        if n:
            stage_c(*steps[n - 1])
        stage_b(s, p)
        if n > 1:
            stage_d(*steps[n - 2])
    stage_d(*steps[-2])
    stage_c(*steps[-1])
    stage_d(*steps[-1])

    for s, p in steps:
        zz = order(s)

        @pl.when(zz // (nz // 2) == c)
        def _():
            finish(s, p).wait_recv()

        @pl.when(zz // (nz // 2) != c)
        def _():
            finish(s, p).wait_send()
    outs = [pltpu.make_async_copy(
        fin.at[k, h], out.at[pl.ds(h * half, half), pl.ds(k * blk, blk)], loc.at[k * 2 + h])
        for k in range(nz // 2) for h in range(2)]
    for copy in outs:
        copy.start()
    for w in range(2):
        swap[w].wait_send()
        for s in range(nz):
            for p in pieces(w):
                send(w, order(s), p, "wait")
    for s, p in steps:
        d2d(s, p).wait_send()
        to_first(s, p, 0).wait_send()
        to_first(s, p, 1).wait_send()
        to_second(s, p).wait_send()
    for copy in outs:
        copy.wait()


def fused(nz, normed, up, down):
    rows, d = normed.shape
    wide = up.shape[1] // 4
    half, blk = rows // 2, d // nz
    sem = pltpu.SemaphoreType.DMA
    return pl.pallas_call(
        functools.partial(kernel, nz),
        out_shape=jax.ShapeDtypeStruct((rows, d // 2), BF16),
        in_specs=[pl.BlockSpec(memory_space=pl.ANY)] * 3,
        out_specs=pl.BlockSpec(memory_space=pl.ANY),
        scratch_shapes=[
            pltpu.VMEM((nz, 4, 2, half, blk), BF16),
            pltpu.VMEM((4, 2, half, wide), F32),
            pltpu.VMEM((4, 2, half, wide), BF16),
            pltpu.VMEM((nz, blk, wide), BF16),
            pltpu.VMEM((nz, wide, blk), BF16),
            pltpu.VMEM((nz, 4, half, blk), BF16),
            pltpu.VMEM((nz, 2, half, blk), BF16),
            pltpu.VMEM((nz, half, blk), BF16),
            pltpu.VMEM((nz // 2, 2, half, blk), BF16),
            sem((2 * nz + 2,)), sem((6,)), sem((6,)), sem((2,)), sem((2,)),
            sem((2, 2, nz, 2)), sem((2, nz, 2)), sem((nz, 2)), sem((nz, 2)),
            sem((nz, 2, 2)), sem((nz, 2, 2)), sem((nz, 2)), sem((nz, 2)), sem((nz, 2)),
            sem((nz, 2)),
        ],
        compiler_params=pltpu.CompilerParams(
            collective_id=0, has_side_effects=True, vmem_limit_bytes=60 * 2**20),
    )(normed, up, down)


def spread(normed, up_weight, down_weight):
    n_rep = lax.axis_size("rep")
    rep = lax.axis_index("rep")
    ff = up_weight.shape[1] // n_rep
    up = lax.all_gather(
        lax.dynamic_slice_in_dim(up_weight, rep * ff, ff, 1), "fs", axis=0, tiled=True)
    down = lax.all_gather(
        lax.dynamic_slice_in_dim(down_weight, rep * ff, ff, 0), "fs", axis=1, tiled=True)
    normed = lax.all_gather(normed, "rep", axis=0, tiled=True)
    pre = jnp.dot(normed, up, preferred_element_type=F32)
    hidden = jnp.square(jax.nn.relu(pre)).astype(BF16)
    terms = jnp.dot(hidden, down, preferred_element_type=F32).astype(BF16)
    summed = lax.psum_scatter(terms, "tp", scatter_dimension=1, tiled=True)
    return lax.psum_scatter(summed, "rep", scatter_dimension=0, tiled=True)


def local(tokens, norm_gain, up_weight, down_weight):
    xf = tokens.astype(F32)
    inv_rms = lax.rsqrt(jnp.mean(xf * xf, axis=-1, keepdims=True) + 1e-06)
    normed = (xf * inv_rms * norm_gain).astype(BF16)
    n_rep, n_fs, n_tp = (lax.axis_size(a) for a in ("rep", "fs", "tp"))
    if n_rep == 2 and n_tp == 2 and n_fs % 4 == 0:
        summed = fused(n_fs // 2, normed, up_weight, down_weight)
    else:
        summed = spread(normed, up_weight, down_weight)
    summed = summed.astype(F32)
    width = summed.shape[1]
    own_cols = lax.dynamic_slice_in_dim(xf, lax.axis_index("tp") * width, width, 1)
    return (own_cols + summed).astype(BF16)


def solution(mesh):
    placed = (P(("rep", "fs"), None), P(), P("fs", "tp"), P("tp", "fs"))
    return jax.shard_map(
        local, mesh=mesh, in_specs=placed, out_specs=P(("rep", "fs"), "tp"), check_vma=False
    )
```
